32 devices in a mesh: sp: 8 (over z, x), tp: 4 (over y, core).
Axes of the slice: x: 2, y: 2, z: 4, core: 2. Of those that a mesh axis runs over, the one named last changes fastest.
Arguments:
- tokens: bfloat16 [5120, 2048], P(('sp', 'tp')), may hold values from -44 to 44
- in_gain: float32 [2048], replicated, may hold values from 0.1 to 1.9
- w_x: bfloat16 [2048, 2048], P('sp', 'tp'), may hold values from -0.125 to 0.125
- w_z: bfloat16 [2048, 2048], P('sp', 'tp'), may hold values from -0.125 to 0.125
- w_b: bfloat16 [2048, 1024], P('sp', 'tp'), may hold values from -0.125 to 0.125
- w_c: bfloat16 [2048, 1024], P('sp', 'tp'), may hold values from -0.125 to 0.125
- w_dt: bfloat16 [2048, 32], replicated, may hold values from -0.125 to 0.125
- conv_x: float32 [4, 2048], replicated, may hold values from -3 to 3
- conv_b: float32 [4, 1024], replicated, may hold values from -3 to 3
- conv_c: float32 [4, 1024], replicated, may hold values from -3 to 3
- dt_bias: float32 [32], replicated, may hold values from -15 to -3.5
- a_log: float32 [32], replicated, may hold values from -0.5 to 0.5
- out_gain: float32 [2048], replicated, may hold values from 0.1 to 1.9
- w_out: bfloat16 [2048, 2048], P('tp', 'sp'), may hold values from -0.125 to 0.125
Outputs:
- mixer_out: bfloat16 [5120, 2048], P(('sp', 'tp'))
The draws below stay inside these ranges and needn't reach their ends.
All inputs are finite; a program needn't handle non-finite values.
Results may differ from the reference program's by a relative error of at most 0.015.
Values may be sent and summed in bfloat16 or wider, within the bound.
A program may use at most 128 MiB of HBM per device.

```python
import math
import jax
import jax.numpy as jnp
from jax import lax

D = 2048
HEADS = 32
GROUPS = 8
HEAD_DIM = 64
STATE = 128
CONV = 4
BLOCK = 128
SEG = 640
INNER = 2048
LENGTH = 5120
N_TP = 4


def draw_tokens(key, part):
    base_key, lift_key, axis_key = jax.random.split(key, 3)
    segments = LENGTH // SEG
    base_rows = jnp.clip(jax.random.normal(base_key, (segments, SEG, D), jnp.float32), -6.0, 6.0)
    block_lift = jax.random.uniform(lift_key, (segments, 1, 1), jnp.float32, -1.2, 1.2)
    direction = jnp.clip(jax.random.normal(axis_key, (1, 1, D), jnp.float32), -4.0, 4.0)
    values = (base_rows + block_lift * direction).reshape(LENGTH, D)
    return values.astype(jnp.bfloat16)


def draw_dt_bias(key, part):
    pick_key, jitter_key = jax.random.split(key)
    slow_share = 0.5
    slow_heads = jax.random.uniform(pick_key, (HEADS,), jnp.float32) < slow_share
    jitter = jax.random.uniform(jitter_key, (HEADS,), jnp.float32, -0.5, 0.5)
    slow_value = -math.log(LENGTH) - 0.3 + jitter
    fast_value = -4.0 + jitter
    return jnp.where(slow_heads, slow_value, fast_value).astype(jnp.float32)


def block_scale(rng, shape, cuts, smallest, high):
    loudness = 1.0
    for position, shards_of in cuts:
        steps = jax.random.uniform(jax.random.fold_in(jax.random.fold_in(rng, 6), position), (shards_of,), jnp.float32, smallest / len(cuts), high / len(cuts))
        loudness = loudness * jnp.repeat(jnp.exp(steps), shape[position] // shards_of).reshape((-1,) + (1,) * (len(shape) - 1 - position))
    return loudness


def normal_values(key, shape, deviation, bound, shards=(), kind=jnp.bfloat16):
    drawn = jax.random.normal(key, shape, jnp.float32) * deviation
    if len(shards) > 0:
        drawn = block_scale(key, shape, shards, -0.22, 0.18) * drawn
    return jnp.clip(drawn, min=-bound, max=bound).astype(kind)


def setup_inputs(seed: int = 0) -> dict:
    key_of = jax.random.split(jax.random.key(seed), 15)
    return {
        "tokens": draw_tokens(jax.random.fold_in(key_of[14], 71), 0),
        "in_gain": jnp.clip(1.0 + 0.18 * jax.random.normal(key_of[1], (D,), jnp.float32), 0.1, 1.9),
        "w_x": normal_values(key_of[2], (D, INNER), D ** -0.5, 0.125, ((0, 8), (1, 4))),
        "w_z": normal_values(key_of[3], (D, INNER), D ** -0.5, 0.125, ((0, 8), (1, 4))),
        "w_b": normal_values(key_of[4], (D, GROUPS * STATE), D ** -0.5, 0.125, ((0, 8), (1, 4))),
        "w_c": normal_values(key_of[5], (D, GROUPS * STATE), D ** -0.5, 0.125, ((0, 8), (1, 4))),
        "w_dt": normal_values(key_of[6], (D, HEADS), D ** -0.5, 0.125),
        "conv_x": normal_values(key_of[7], (CONV, INNER), CONV ** -0.5, 3.0, (), jnp.float32),
        "conv_b": normal_values(key_of[8], (CONV, GROUPS * STATE), CONV ** -0.5, 3.0, (), jnp.float32),
        "conv_c": normal_values(key_of[9], (CONV, GROUPS * STATE), CONV ** -0.5, 3.0, (), jnp.float32),
        "dt_bias": draw_dt_bias(jax.random.fold_in(key_of[14], 71), 0),
        "a_log": jnp.clip(jax.random.uniform(key_of[11], (HEADS,), jnp.float32, -0.5, 0.5), -0.5, 0.5),
        "out_gain": jnp.clip(1.0 + 0.18 * jax.random.normal(key_of[12], (INNER,), jnp.float32), 0.1, 1.9),
        "w_out": normal_values(key_of[13], (INNER, D), INNER ** -0.5, 0.125, ((0, 4), (1, 8))),
    }


EPS = 1e-06
HIGH = lax.Precision.HIGHEST

def inverse_rms(values):
    return lax.rsqrt(lax.optimization_barrier(jnp.mean(values * values, axis=-1, keepdims=True)) + EPS)

def causal_conv(prev_rows, new_rows, kernel):
    joined = jnp.concatenate([prev_rows, new_rows], axis=0).astype(jnp.float32)
    row_count = new_rows.shape[0]
    summed = jnp.zeros(new_rows.shape, jnp.float32)
    for offset in range(CONV):
        summed = summed + kernel[offset] * joined[offset:offset + row_count]
    return jax.nn.silu(summed)

def project(normed, weight):
    return jnp.dot(normed.astype(jnp.float32), weight, precision=HIGH, preferred_element_type=jnp.float32)

def reference(tokens, in_gain, w_x, w_z, w_b, w_c, w_dt, conv_x, conv_b, conv_c, dt_bias, a_log, out_gain, w_out):
    group_heads = HEADS // GROUPS
    share_width = INNER // N_TP
    conv_keep = CONV - 1
    weights_in = tuple((weight.astype(jnp.float32) for weight in (w_x, w_z, w_b, w_c, w_dt)))
    weight_out = w_out.astype(jnp.float32)
    decay_rates = jnp.exp(a_log)
    causal = lax.broadcasted_iota(jnp.int32, (BLOCK, BLOCK), 0) >= lax.broadcasted_iota(jnp.int32, (BLOCK, BLOCK), 1)
    lower_ones = causal.astype(jnp.float32)

    def advance(carried_in, block_rows):
        run_state, prev_x, prev_b, prev_c = carried_in
        values = block_rows.astype(jnp.float32)
        normed = (values * inverse_rms(values) * in_gain).astype(jnp.bfloat16)
        proj_x, proj_z, proj_b, proj_c = [project(normed, weight).astype(jnp.bfloat16) for weight in weights_in[:4]]
        dt_raw = project(normed, weights_in[4])
        conv_xs = causal_conv(prev_x, proj_x, conv_x)
        conv_bs = causal_conv(prev_b, proj_b, conv_b)
        conv_cs = causal_conv(prev_c, proj_c, conv_c)
        step_size = jax.nn.softplus(dt_raw + dt_bias)
        log_decay = -step_size * decay_rates
        cum_decay = jnp.dot(lower_ones, log_decay, precision=HIGH)
        scaled_x = conv_xs.reshape(BLOCK, HEADS, HEAD_DIM) * step_size[:, :, None]
        b_heads = jnp.repeat(conv_bs.reshape(BLOCK, GROUPS, STATE), group_heads, axis=1)
        c_heads = jnp.repeat(conv_cs.reshape(BLOCK, GROUPS, STATE), group_heads, axis=1)
        scores = jnp.einsum('lhn,shn->hls', c_heads, b_heads, precision=HIGH)
        decay_gap = cum_decay.T[:, :, None] - cum_decay.T[:, None, :]
        within = jnp.where(causal, jnp.exp(jnp.where(causal, decay_gap, 0.0)), 0.0) * scores
        inside = jnp.einsum('hls,shp->lhp', within, scaled_x, precision=HIGH)
        carried = jnp.einsum('lhn,hpn->lhp', c_heads, run_state, precision=HIGH) * jnp.exp(cum_decay)[:, :, None]
        block_total = cum_decay[BLOCK - 1]
        tail_weight = jnp.exp(block_total[None, :] - cum_decay)
        new_state = run_state * jnp.exp(block_total)[:, None, None] + jnp.einsum('lhp,lhn->hpn', scaled_x * tail_weight[:, :, None], b_heads, precision=HIGH)
        gated_out = (inside + carried).reshape(BLOCK, INNER) * jax.nn.silu(proj_z.astype(jnp.float32))
        grouped = gated_out.reshape(BLOCK, GROUPS, INNER // GROUPS)
        mixed_rows = ((grouped * inverse_rms(grouped)).reshape(BLOCK, INNER) * out_gain).astype(jnp.bfloat16)
        summed = jnp.zeros((BLOCK, D), jnp.float32)
        for share_index in range(N_TP):
            columns = mixed_rows[:, share_index * share_width:(share_index + 1) * share_width]
            partial_sum = project(columns, weight_out[share_index * share_width:(share_index + 1) * share_width]).astype(jnp.bfloat16)
            summed = summed + lax.optimization_barrier(partial_sum).astype(jnp.float32)
        new_carry = (new_state, proj_x[BLOCK - conv_keep:], proj_b[BLOCK - conv_keep:], proj_c[BLOCK - conv_keep:])
        return (new_carry, summed.astype(jnp.bfloat16))
    initial = (jnp.zeros((HEADS, HEAD_DIM, STATE), jnp.float32), jnp.zeros((conv_keep, INNER), jnp.bfloat16), jnp.zeros((conv_keep, GROUPS * STATE), jnp.bfloat16), jnp.zeros((conv_keep, GROUPS * STATE), jnp.bfloat16))
    unused, outputs = lax.scan(advance, initial, tokens.reshape(LENGTH // BLOCK, BLOCK, D))
    return outputs.reshape(LENGTH, D)
```

```python
import jax
import jax.numpy as jnp
from jax import lax
from jax.experimental import pallas as pl
from jax.experimental.pallas import tpu as pltpu
from jax.sharding import PartitionSpec as P

HEAD_DIM = 64
STATE = 128
CONV = 4
BLOCK = 128


EPS = 1e-06
HIGH = lax.Precision.HIGHEST


def carried_in(part, axis, combine, identity):
    place = lax.axis_index(axis)
    gathered = jax.tree.map(lambda a: lax.all_gather(a, axis), part)
    state = jax.tree.map(lambda a, e: jnp.zeros_like(a) + jnp.asarray(e, a.dtype), part, identity)

    def one(lap, state):
        return combine(
            state, jax.tree.map(lambda a: lax.dynamic_index_in_dim(a, lap, 0, False), gathered)
        )

    return lax.fori_loop(0, place, one, state)


def from_behind(value, axis, steps):
    count = lax.axis_size(axis)
    first, last = (max(0, -steps), min(count, count - steps))
    return lax.ppermute(value, axis, [(source, source + steps) for source in range(first, last)])


def inverse_rms(values):
    return lax.rsqrt(jnp.mean(values * values, axis=-1, keepdims=True) + EPS)


def causal_conv(prev_rows, new_rows, kernel):
    joined = jnp.concatenate([prev_rows, new_rows], axis=0).astype(jnp.float32)
    row_count = new_rows.shape[0]
    summed = jnp.zeros(new_rows.shape, jnp.float32)
    for offset in range(kernel.shape[0]):
        summed = summed + kernel[offset] * joined[offset : offset + row_count]
    return jax.nn.silu(summed)


def fold_single(gathered):

    def fold_step(total_part, rows_part, first_row):
        return jnp.dot(gathered, rows_part, preferred_element_type=jnp.float32)

    return fold_step


def fold_products(gathered, totals, weight_rows, first_row):
    single = fold_single(gathered)
    return tuple(
        (
            single(total_part, rows_part, first_row)
            for total_part, rows_part in zip(totals, weight_rows)
        )
    )


def inner_part(cum_decay, b_rows, c_rows, scaled_x, causal):
    scores = jnp.einsum("blgn,bsgn->bgls", c_rows, b_rows, precision=HIGH)
    decay_gap = cum_decay[:, :, None] - cum_decay[:, None, :]
    causal_mask = causal[None, :, :, None, None]
    within = jnp.where(causal_mask, jnp.exp(jnp.where(causal_mask, decay_gap, 0.0)), 0.0)
    return jnp.einsum("bgls,blsgh,bsghp->blghp", scores, within, scaled_x, precision=HIGH)


def carried_part(c_rows, states, cum_decay):
    return jnp.einsum("blgn,bghpn,blgh->blghp", c_rows, states, jnp.exp(cum_decay), precision=HIGH)


def run_blocks(block_states, block_decay, start_state):

    def advance(run_state, inputs):
        fresh_state, factor = inputs
        return (run_state * factor[:, :, None, None] + fresh_state, run_state)

    final_state, entering = lax.scan(advance, start_state, (block_states, block_decay))
    return (entering, final_state)


def chain(earlier, later):
    return (earlier[0] * later[0], earlier[1] * later[0][:, :, None, None] + later[1])


def carry_in(total_decay, final_state):
    identity = (jnp.ones_like(total_decay), jnp.zeros_like(final_state))
    before = carried_in((total_decay, final_state), "sp", chain, identity)
    return before[1]


def body(
    tokens,
    in_gain,
    w_x,
    w_z,
    w_b,
    w_c,
    w_dt,
    conv_x,
    conv_b,
    conv_c,
    dt_bias,
    a_log,
    out_gain,
    w_out,
):
    share_index = lax.axis_index("tp")
    width_x = w_x.shape[1]
    width_b = w_b.shape[1]
    heads_here = width_x // HEAD_DIM
    groups_here = width_b // STATE
    group_heads = heads_here // groups_here
    kernel_x = lax.dynamic_slice_in_dim(conv_x, share_index * width_x, width_x, 1)
    kernel_b = lax.dynamic_slice_in_dim(conv_b, share_index * width_b, width_b, 1)
    kernel_c = lax.dynamic_slice_in_dim(conv_c, share_index * width_b, width_b, 1)
    bias_here = lax.dynamic_slice_in_dim(dt_bias, share_index * heads_here, heads_here, 0)
    rate_here = jnp.exp(lax.dynamic_slice_in_dim(a_log, share_index * heads_here, heads_here, 0))
    gain_here = lax.dynamic_slice_in_dim(out_gain, share_index * width_x, width_x, 0)
    dt_weight = lax.dynamic_slice_in_dim(w_dt, share_index * heads_here, heads_here, 1)
    values = tokens.astype(jnp.float32)
    normed = (values * inverse_rms(values) * in_gain).astype(jnp.bfloat16)
    gathered = lax.all_gather(normed, "tp", axis=0, tiled=True)
    seg_rows = gathered.shape[0]
    blocks = seg_rows // BLOCK
    empty_x = jnp.zeros((seg_rows, width_x), jnp.float32)
    empty_b = jnp.zeros((seg_rows, width_b), jnp.float32)
    projected = fold_products(
        gathered,
        (empty_x, empty_x, empty_b, empty_b),
        (
            lax.all_gather(w_x, "sp", axis=0, tiled=True),
            lax.all_gather(w_z, "sp", axis=0, tiled=True),
            lax.all_gather(w_b, "sp", axis=0, tiled=True),
            lax.all_gather(w_c, "sp", axis=0, tiled=True),
        ),
        jnp.int32(0),
    )
    proj_x, gate_rows, proj_b, proj_c = [
        summed_part.astype(jnp.bfloat16) for summed_part in projected
    ]
    dt_raw = jnp.dot(gathered, dt_weight, preferred_element_type=jnp.float32)
    conv_keep = CONV - 1
    tail_start = seg_rows - conv_keep
    prev_x, prev_b, prev_c = from_behind(
        (proj_x[tail_start:], proj_b[tail_start:], proj_c[tail_start:]), "sp", 1
    )
    conv_xs = causal_conv(prev_x, proj_x, kernel_x)
    conv_bs = causal_conv(prev_b, proj_b, kernel_b)
    conv_cs = causal_conv(prev_c, proj_c, kernel_c)
    step_size = jax.nn.softplus(dt_raw + bias_here)
    log_decay = (-step_size * rate_here).reshape(blocks, BLOCK, groups_here, group_heads)
    causal = lax.broadcasted_iota(jnp.int32, (BLOCK, BLOCK), 0) >= lax.broadcasted_iota(
        jnp.int32, (BLOCK, BLOCK), 1
    )
    cum_decay = jnp.einsum("ls,bsgh->blgh", causal.astype(jnp.float32), log_decay, precision=HIGH)
    scaled_x = (conv_xs.reshape(seg_rows, heads_here, HEAD_DIM) * step_size[:, :, None]).reshape(
        blocks, BLOCK, groups_here, group_heads, HEAD_DIM
    )
    b_rows = conv_bs.reshape(blocks, BLOCK, groups_here, STATE)
    c_rows = conv_cs.reshape(blocks, BLOCK, groups_here, STATE)
    block_total = cum_decay[:, BLOCK - 1]
    tail_weight = jnp.exp(block_total[:, None] - cum_decay)
    block_states = jnp.einsum(
        "blgn,blgh,blghp->bghpn", b_rows, tail_weight, scaled_x, precision=HIGH
    )
    block_decay = jnp.exp(block_total)
    total_decay = jnp.exp(jnp.sum(block_total, axis=0))
    start_state = jnp.zeros(block_states.shape[1:], jnp.float32)
    entering, final_state = run_blocks(block_states, block_decay, start_state)
    incoming = carry_in(total_decay, final_state)

    def per_block(run_state, inputs):
        cum_here, b_here, c_here, x_here, fresh_state, factor = inputs
        output = inner_part(cum_here[None], b_here[None], c_here[None], x_here[None], causal)[0]
        output = output + carried_part(c_here[None], run_state[None], cum_here[None])[0]
        return (run_state * factor[:, :, None, None] + fresh_state, output)

    unused, heads_out = lax.scan(
        per_block, incoming, (cum_decay, b_rows, c_rows, scaled_x, block_states, block_decay)
    )
    gated_out = heads_out.reshape(seg_rows, width_x) * jax.nn.silu(gate_rows.astype(jnp.float32))
    grouped = gated_out.reshape(seg_rows, groups_here, width_x // groups_here)
    mixed_rows = ((grouped * inverse_rms(grouped)).reshape(seg_rows, width_x) * gain_here).astype(
        jnp.bfloat16
    )
    partial_sum = jnp.dot(
        mixed_rows,
        lax.all_gather(w_out, "sp", axis=1, tiled=True),
        preferred_element_type=jnp.float32,
    )
    return lax.psum_scatter(partial_sum.astype(jnp.bfloat16), "tp", scatter_dimension=0, tiled=True)


MESH = pl.DeviceIdType.MESH
BF16 = jnp.bfloat16
F32 = jnp.float32
HALO = 16


def mixer_kernel(
    n_sp,
    n_tp,
    tok_ref,
    in_gain_ref,
    w_x_ref,
    w_bc_ref,
    w_z_ref,
    w_o_ref,
    w_dt_ref,
    taps_x_ref,
    taps_bc_ref,
    bias_ref,
    rate_ref,
    gain_ref,
    out_ref,
    nall,
    gath,
    gath_o,
    proj,
    scaled,
    bc_rows,
    log_step,
    cum_seg,
    heads_cum,
    entering,
    state,
    y_buf,
    mixed,
    part,
    pair_in,
    slot_f,
    slot_a,
    tok_send,
    tok_recv,
    halo_send,
    halo_recv,
    z_send,
    x_send,
    w_recv,
    own_sem,
    st_send,
    st_recv,
    rs_send,
    rs_recv,
):
    sp = lax.axis_index("sp")
    tp = lax.axis_index("tp")
    share = tok_ref.shape[0]
    seg_rows = share * n_tp
    blocks = seg_rows // BLOCK
    width = w_x_ref.shape[1]
    half = width // 2
    heads_here = width // HEAD_DIM
    groups_here = half // STATE
    group_heads = heads_here // groups_here
    group_width = width // groups_here
    depth = w_x_ref.shape[0]
    n_z = n_sp // 2
    beside = sp + 1 - 2 * lax.rem(sp, 2)
    own_refs = (w_x_ref, w_bc_ref, w_z_ref, w_o_ref)

    def remote(src, dst, send, recv, where):
        return pltpu.make_async_remote_copy(
            src_ref=src, dst_ref=dst, send_sem=send, recv_sem=recv, device_id=where,
            device_id_type=MESH,
        )

    def place(chunk, source):
        if chunk == 3:
            cols = w_o_ref.shape[1]
            return gath_o.at[:, pl.ds(pl.multiple_of(source * cols, cols), cols)]
        return gath.at[chunk, pl.ds(pl.multiple_of(source * depth, depth), depth), :]

    values = tok_ref[...].astype(F32)
    normed = (values * inverse_rms(values) * in_gain_ref[...]).astype(BF16)

    def token_rows(index):
        return nall.at[pl.ds(pl.multiple_of(HALO + index * share, 16), share), :]

    token_rows(tp)[...] = normed

    def token_copy(step):
        return remote(
            token_rows(tp), token_rows(tp), tok_send.at[step - 1], tok_recv.at[tp],
            (sp, lax.rem(tp + step, n_tp)),
        )

    def halo_copy(target):
        return remote(
            nall.at[pl.ds(seg_rows, HALO), :], nall.at[pl.ds(0, HALO), :], halo_send.at[target],
            halo_recv.at[0], (lax.rem(sp + 1, n_sp), target),
        )

    @pl.when(tp == n_tp - 1)
    def _():
        for target in range(n_tp):
            halo_copy(target).start()

    def z_copy(chunk, step):
        return remote(
            own_refs[chunk], place(chunk, sp), z_send.at[chunk, step], w_recv.at[chunk, sp],
            (lax.rem(sp + 2 * step, n_sp), tp),
        )

    def x_copy(chunk, step):
        source = lax.rem(sp + n_sp - 2 * step, n_sp)
        src = own_refs[chunk] if step == 0 else place(chunk, source)
        return remote(
            src, place(chunk, source), x_send.at[chunk, step], w_recv.at[chunk, source],
            (beside, tp),
        )

    def arrival(chunk, source):
        return remote(
            own_refs[chunk], place(chunk, source), z_send.at[chunk, 0], w_recv.at[chunk, source],
            (beside, tp),
        )

    def own_copy(chunk):
        return pltpu.make_async_copy(own_refs[chunk], place(chunk, sp), own_sem.at[chunk])

    for chunk in range(4):
        x_copy(chunk, 0).start()
        for step in range(1, n_z):
            z_copy(chunk, step).start()
        if chunk == 0:
            for step in range(1, n_tp):
                token_copy(step).start()
        own_copy(chunk).start()

    def forward(chunk):
        for step in range(1, n_z):
            source = lax.rem(sp + n_sp - 2 * step, n_sp)
            arrival(chunk, source).wait_recv()
            x_copy(chunk, step).start()

    def finish(chunk):
        own_copy(chunk).wait()
        for step in range(n_z):
            arrival(chunk, lax.rem(beside + n_sp - 2 * step, n_sp)).wait_recv()

    forward(0)
    for step in range(1, n_tp):
        source = lax.rem(tp + n_tp - step, n_tp)
        remote(
            token_rows(source), token_rows(source), tok_send.at[0], tok_recv.at[source],
            (sp, source),
        ).wait_recv()
    halo_copy(0).wait_recv()

    @pl.when(tp == n_tp - 1)
    def _():
        for target in range(n_tp):
            halo_copy(target).wait_send()

    for step in range(1, n_tp):
        token_copy(step).wait_send()

    @pl.when(sp == 0)
    def _():
        nall[pl.ds(0, HALO), :] = jnp.zeros((HALO, nall.shape[1]), BF16)

    raw = jnp.dot(nall[pl.ds(HALO, seg_rows), :], w_dt_ref[...], preferred_element_type=F32)
    raw = raw + bias_ref[...]
    log_step[...] = jnp.maximum(raw, 0.0) + jnp.log1p(jnp.exp(-jnp.abs(raw)))
    lanes = log_step.shape[1]
    spread = (
        lax.broadcasted_iota(jnp.int32, (lanes, width), 0)
        == lax.broadcasted_iota(jnp.int32, (lanes, width), 1) // HEAD_DIM
    ).astype(F32)
    causal = lax.broadcasted_iota(jnp.int32, (BLOCK, BLOCK), 0) >= lax.broadcasted_iota(
        jnp.int32, (BLOCK, BLOCK), 1
    )

    def project(chunk):
        proj[...] = (
            jnp.dot(nall[...], gath[chunk], preferred_element_type=F32).astype(BF16).astype(F32)
        )

    def conv(block, taps):
        summed = jnp.zeros((BLOCK, width), F32)
        start = block * BLOCK + HALO - (CONV - 1)
        for offset in range(CONV):
            summed = summed + taps[offset : offset + 1, :] * proj[
                start + offset : start + offset + BLOCK, :
            ]
        return summed / (1.0 + jnp.exp(-summed))

    forward(1)
    finish(0)
    project(0)
    for block in range(blocks):
        rows = pl.ds(block * BLOCK, BLOCK)
        step_here = jnp.dot(log_step[rows, :], spread, precision=HIGH, preferred_element_type=F32)
        scaled[rows, :] = conv(block, taps_x_ref[...]) * step_here

    finish(1)
    project(1)
    for block in range(blocks):
        rows = pl.ds(block * BLOCK, BLOCK)
        bc_rows[rows, :] = conv(block, taps_bc_ref[...]).astype(BF16)

    def rows_of(block):
        return pl.ds(pl.multiple_of(block * BLOCK, BLOCK), BLOCK)

    state[...] = jnp.zeros_like(state)
    tri = causal.astype(F32)

    def states_of(block, total):
        rows = rows_of(block)
        log_rate = -log_step[rows, :] * rate_ref[...]
        cum = jnp.dot(tri, log_rate, precision=HIGH, preferred_element_type=F32)
        heads_cum[rows, :] = cum
        wide = jnp.dot(cum, spread, precision=HIGH, preferred_element_type=F32)
        cum_seg[rows, :] = wide
        last = wide[BLOCK - 1 : BLOCK, :]
        weighted = (scaled[rows, :] * jnp.exp(last - wide)).astype(BF16)
        old = state[...]
        entering[block] = old.astype(BF16)
        decay = jnp.exp(last)
        for group in range(groups_here):
            cols = slice(group * group_width, (group + 1) * group_width)
            b_here = bc_rows[rows, group * STATE : (group + 1) * STATE]
            fresh = lax.dot_general(
                b_here, weighted[:, cols], (((0,), (0,)), ((), ())), preferred_element_type=F32
            )
            state[:, cols] = old[:, cols] * decay[:, cols] + fresh
        return total + last

    total = lax.fori_loop(0, blocks, states_of, jnp.zeros((1, width), F32))
    slot_f[sp] = state[...].astype(BF16)
    slot_a[sp] = jnp.broadcast_to(jnp.exp(total), slot_a.shape[1:])

    def state_copies(source, target):
        return (
            remote(
                slot_f.at[source], slot_f.at[source], st_send.at[0, target],
                st_recv.at[0, source], (target, tp),
            ),
            remote(
                slot_a.at[source], slot_a.at[source], st_send.at[1, target],
                st_recv.at[1, source], (target, tp),
            ),
        )

    for target in range(1, n_sp):
        @pl.when(target > sp)
        def _():
            for copy in state_copies(sp, target):
                copy.start()

    forward(2)

    def outputs_of(block, carry):
        rows = rows_of(block)
        cum = heads_cum[rows, :]
        cum_t = cum.T
        wide = jnp.exp(cum_seg[rows, :])
        x_here = scaled[rows, :].astype(BF16)
        before = entering[block]
        for group in range(groups_here):
            cols = slice(group * group_width, (group + 1) * group_width)
            b_here = bc_rows[rows, group * STATE : (group + 1) * STATE]
            c_here = bc_rows[rows, half + group * STATE : half + (group + 1) * STATE]
            scores = lax.dot_general(
                c_here, b_here, (((1,), (1,)), ((), ())), preferred_element_type=F32
            )
            parts = []
            for index in range(group * group_heads, (group + 1) * group_heads):
                gap = cum[:, index : index + 1] - cum_t[index : index + 1, :]
                within = jnp.where(causal, jnp.exp(jnp.where(causal, gap, 0.0)), 0.0)
                parts.append(
                    jnp.dot(
                        (scores * within).astype(BF16),
                        x_here[:, index * HEAD_DIM : (index + 1) * HEAD_DIM],
                        preferred_element_type=F32,
                    )
                )
            inner = jnp.concatenate(parts, axis=1)
            carried = jnp.dot(c_here, before[:, cols], preferred_element_type=F32)
            y_buf[rows, cols] = inner + carried * wide[:, cols]
        return carry

    lax.fori_loop(0, blocks, outputs_of, 0)
    forward(3)
    finish(2)
    project(2)

    for source in range(n_sp - 1):
        @pl.when(source < sp)
        def _():
            for copy in state_copies(source, sp):
                copy.wait_recv()

    state[...] = jnp.zeros_like(state)

    def combine(source, carry):
        state[...] = state[...] * slot_a[source, 0:1, :] + slot_f[source].astype(F32)
        return carry

    lax.fori_loop(0, sp, combine, 0)

    def gate_of(block, before):
        rows = rows_of(block)
        wide = cum_seg[rows, :]
        decay = jnp.exp(before + wide)
        gate = proj[pl.ds(pl.multiple_of(block * BLOCK + HALO, 16), BLOCK), :]
        silu = gate / (1.0 + jnp.exp(-gate))
        for group in range(groups_here):
            cols = slice(group * group_width, (group + 1) * group_width)
            c_here = bc_rows[rows, half + group * STATE : half + (group + 1) * STATE]
            carried = jnp.dot(c_here, state[:, cols].astype(BF16), preferred_element_type=F32)
            gated = (y_buf[rows, cols] + carried * decay[:, cols]) * silu[:, cols]
            mixed[rows, cols] = (gated * inverse_rms(gated) * gain_ref[:, cols]).astype(BF16)
        return before + wide[BLOCK - 1 : BLOCK, :]

    lax.fori_loop(0, blocks, gate_of, jnp.zeros((1, width), F32))
    finish(3)

    partner = tp + 1 - 2 * lax.rem(tp, 2)
    across = lax.rem(tp + 2, n_tp)
    across_partner = lax.rem(partner + 2, n_tp)

    def product(index):
        rows = pl.ds(pl.multiple_of(index * share, 16), share)
        return jnp.dot(mixed[rows, :], gath_o[...], preferred_element_type=F32).astype(BF16)

    def pair_copy(slot, where):
        return remote(
            part.at[slot], pair_in.at[slot], rs_send.at[slot], rs_recv.at[slot], (sp, where)
        )

    part[0] = product(across_partner)
    pair_copy(0, partner).start()
    part[1] = product(partner)
    pair_copy(1, partner).start()
    mine = product(across)
    pair_copy(0, partner).wait_recv()
    part[2] = (mine.astype(F32) + pair_in[0].astype(F32)).astype(BF16)
    pair_copy(2, across).start()
    kept = product(tp).astype(F32)
    pair_copy(1, partner).wait_recv()
    kept = kept + pair_in[1].astype(F32)
    pair_copy(2, across).wait_recv()
    out_ref[...] = (kept + pair_in[2].astype(F32)).astype(BF16)

    pair_copy(0, partner).wait_send()
    pair_copy(1, partner).wait_send()
    pair_copy(2, across).wait_send()
    for chunk in range(4):
        for step in range(n_z):
            x_copy(chunk, step).wait_send()
        for step in range(1, n_z):
            z_copy(chunk, step).wait_send()
    for target in range(1, n_sp):
        @pl.when(target > sp)
        def _():
            for copy in state_copies(sp, target):
                copy.wait_send()


def fused_body(
    tokens, in_gain, w_x, w_z, w_b, w_c, w_dt, conv_x, conv_b, conv_c, dt_bias, a_log, out_gain,
    w_out,
):
    n_sp = lax.axis_size("sp")
    n_tp = lax.axis_size("tp")
    tp = lax.axis_index("tp")
    share, features = tokens.shape
    seg_rows = share * n_tp
    blocks = seg_rows // BLOCK
    width = w_x.shape[1]
    width_b = w_b.shape[1]
    heads_here = width // HEAD_DIM
    lanes = 128

    def cut(array, size, axis):
        return lax.dynamic_slice_in_dim(array, tp * size, size, axis)

    def wide_row(row):
        return jnp.pad(row, (0, lanes - heads_here))[None]

    w_bc = jnp.concatenate([w_b, w_c], axis=1)
    taps_bc = jnp.concatenate([cut(conv_b, width_b, 1), cut(conv_c, width_b, 1)], axis=1)
    dt_weight = jnp.pad(cut(w_dt, heads_here, 1), ((0, 0), (0, lanes - heads_here)))
    args = (
        tokens,
        in_gain[None],
        w_x,
        w_bc,
        w_z,
        w_out,
        dt_weight,
        cut(conv_x, width, 1),
        taps_bc,
        wide_row(cut(dt_bias, heads_here, 0)),
        wide_row(jnp.exp(cut(a_log, heads_here, 0))),
        cut(out_gain, width, 0)[None],
    )
    dma = pltpu.SemaphoreType.DMA
    vmem = pltpu.VMEM
    n_z = n_sp // 2
    return pl.pallas_call(
        lambda *refs: mixer_kernel(n_sp, n_tp, *refs),
        name="mixer",
        out_shape=jax.ShapeDtypeStruct((share, features), BF16),
        in_specs=[pl.BlockSpec(memory_space=vmem)] * len(args),
        out_specs=pl.BlockSpec(memory_space=vmem),
        scratch_shapes=[
            vmem((seg_rows + HALO, features), BF16),
            vmem((3, features, width), BF16),
            vmem((width, features), BF16),
            vmem((seg_rows + HALO, width), F32),
            vmem((seg_rows, width), F32),
            vmem((seg_rows, 2 * width_b), BF16),
            vmem((seg_rows, lanes), F32),
            vmem((seg_rows, width), F32),
            vmem((seg_rows, lanes), F32),
            vmem((blocks, STATE, width), BF16),
            vmem((STATE, width), F32),
            vmem((seg_rows, width), F32),
            vmem((seg_rows, width), BF16),
            vmem((3, share, features), BF16),
            vmem((3, share, features), BF16),
            vmem((n_sp, STATE, width), BF16),
            vmem((n_sp, 8, width), F32),
            dma((n_tp - 1,)),
            dma((n_tp,)),
            dma((n_tp,)),
            dma((1,)),
            dma((4, n_z)),
            dma((4, n_z)),
            dma((4, n_sp)),
            dma((4,)),
            dma((2, n_sp)),
            dma((2, n_sp)),
            dma((3,)),
            dma((3,)),
        ],
        compiler_params=pltpu.CompilerParams(
            has_side_effects=True, vmem_limit_bytes=60 * 1024 * 1024
        ),
    )(*args)


def solution(mesh):
    in_specs = (
        P(("sp", "tp"), None),
        P(),
        P("sp", "tp"),
        P("sp", "tp"),
        P("sp", "tp"),
        P("sp", "tp"),
        P(),
        P(),
        P(),
        P(),
        P(),
        P(),
        P(),
        P("tp", "sp"),
    )
    out_specs = P(("sp", "tp"), None)
    fits = mesh.shape["tp"] == 4 and mesh.shape["sp"] in (2, 4, 6, 8)
    plan = fused_body if fits else body
    return jax.shard_map(plan, mesh=mesh, in_specs=in_specs, out_specs=out_specs, check_vma=False)
```

```python
import jax
import jax.numpy as jnp
from jax import lax
from jax.experimental import pallas as pl
from jax.experimental.pallas import tpu as pltpu
from jax.sharding import PartitionSpec as P

HEAD_DIM = 64
STATE = 128
CONV = 4
BLOCK = 128


EPS = 1e-06
HIGH = lax.Precision.HIGHEST


def carried_in(part, axis, combine, identity):
    place = lax.axis_index(axis)
    gathered = jax.tree.map(lambda a: lax.all_gather(a, axis), part)
    state = jax.tree.map(lambda a, e: jnp.zeros_like(a) + jnp.asarray(e, a.dtype), part, identity)

    def one(lap, state):
        return combine(
            state, jax.tree.map(lambda a: lax.dynamic_index_in_dim(a, lap, 0, False), gathered)
        )

    return lax.fori_loop(0, place, one, state)


def from_behind(value, axis, steps):
    count = lax.axis_size(axis)
    first, last = (max(0, -steps), min(count, count - steps))
    return lax.ppermute(value, axis, [(source, source + steps) for source in range(first, last)])


def inverse_rms(values):
    return lax.rsqrt(jnp.mean(values * values, axis=-1, keepdims=True) + EPS)


def causal_conv(prev_rows, new_rows, kernel):
    joined = jnp.concatenate([prev_rows, new_rows], axis=0).astype(jnp.float32)
    row_count = new_rows.shape[0]
    summed = jnp.zeros(new_rows.shape, jnp.float32)
    for offset in range(kernel.shape[0]):
        summed = summed + kernel[offset] * joined[offset : offset + row_count]
    return jax.nn.silu(summed)


def fold_single(gathered):

    def fold_step(total_part, rows_part, first_row):
        return jnp.dot(gathered, rows_part, preferred_element_type=jnp.float32)

    return fold_step


def fold_products(gathered, totals, weight_rows, first_row):
    single = fold_single(gathered)
    return tuple(
        (
            single(total_part, rows_part, first_row)
            for total_part, rows_part in zip(totals, weight_rows)
        )
    )


def inner_part(cum_decay, b_rows, c_rows, scaled_x, causal):
    scores = jnp.einsum("blgn,bsgn->bgls", c_rows, b_rows, precision=HIGH)
    decay_gap = cum_decay[:, :, None] - cum_decay[:, None, :]
    causal_mask = causal[None, :, :, None, None]
    within = jnp.where(causal_mask, jnp.exp(jnp.where(causal_mask, decay_gap, 0.0)), 0.0)
    return jnp.einsum("bgls,blsgh,bsghp->blghp", scores, within, scaled_x, precision=HIGH)


def carried_part(c_rows, states, cum_decay):
    return jnp.einsum("blgn,bghpn,blgh->blghp", c_rows, states, jnp.exp(cum_decay), precision=HIGH)


def run_blocks(block_states, block_decay, start_state):

    def advance(run_state, inputs):
        fresh_state, factor = inputs
        return (run_state * factor[:, :, None, None] + fresh_state, run_state)

    final_state, entering = lax.scan(advance, start_state, (block_states, block_decay))
    return (entering, final_state)


def chain(earlier, later):
    return (earlier[0] * later[0], earlier[1] * later[0][:, :, None, None] + later[1])


def carry_in(total_decay, final_state):
    identity = (jnp.ones_like(total_decay), jnp.zeros_like(final_state))
    before = carried_in((total_decay, final_state), "sp", chain, identity)
    return before[1]


def body(
    tokens,
    in_gain,
    w_x,
    w_z,
    w_b,
    w_c,
    w_dt,
    conv_x,
    conv_b,
    conv_c,
    dt_bias,
    a_log,
    out_gain,
    w_out,
):
    share_index = lax.axis_index("tp")
    width_x = w_x.shape[1]
    width_b = w_b.shape[1]
    heads_here = width_x // HEAD_DIM
    groups_here = width_b // STATE
    group_heads = heads_here // groups_here
    kernel_x = lax.dynamic_slice_in_dim(conv_x, share_index * width_x, width_x, 1)
    kernel_b = lax.dynamic_slice_in_dim(conv_b, share_index * width_b, width_b, 1)
    kernel_c = lax.dynamic_slice_in_dim(conv_c, share_index * width_b, width_b, 1)
    bias_here = lax.dynamic_slice_in_dim(dt_bias, share_index * heads_here, heads_here, 0)
    rate_here = jnp.exp(lax.dynamic_slice_in_dim(a_log, share_index * heads_here, heads_here, 0))
    gain_here = lax.dynamic_slice_in_dim(out_gain, share_index * width_x, width_x, 0)
    dt_weight = lax.dynamic_slice_in_dim(w_dt, share_index * heads_here, heads_here, 1)
    values = tokens.astype(jnp.float32)
    normed = (values * inverse_rms(values) * in_gain).astype(jnp.bfloat16)
    gathered = lax.all_gather(normed, "tp", axis=0, tiled=True)
    seg_rows = gathered.shape[0]
    blocks = seg_rows // BLOCK
    empty_x = jnp.zeros((seg_rows, width_x), jnp.float32)
    empty_b = jnp.zeros((seg_rows, width_b), jnp.float32)
    projected = fold_products(
        gathered,
        (empty_x, empty_x, empty_b, empty_b),
        (
            lax.all_gather(w_x, "sp", axis=0, tiled=True),
            lax.all_gather(w_z, "sp", axis=0, tiled=True),
            lax.all_gather(w_b, "sp", axis=0, tiled=True),
            lax.all_gather(w_c, "sp", axis=0, tiled=True),
        ),
        jnp.int32(0),
    )
    proj_x, gate_rows, proj_b, proj_c = [
        summed_part.astype(jnp.bfloat16) for summed_part in projected
    ]
    dt_raw = jnp.dot(gathered, dt_weight, preferred_element_type=jnp.float32)
    conv_keep = CONV - 1
    tail_start = seg_rows - conv_keep
    prev_x, prev_b, prev_c = from_behind(
        (proj_x[tail_start:], proj_b[tail_start:], proj_c[tail_start:]), "sp", 1
    )
    conv_xs = causal_conv(prev_x, proj_x, kernel_x)
    conv_bs = causal_conv(prev_b, proj_b, kernel_b)
    conv_cs = causal_conv(prev_c, proj_c, kernel_c)
    step_size = jax.nn.softplus(dt_raw + bias_here)
    log_decay = (-step_size * rate_here).reshape(blocks, BLOCK, groups_here, group_heads)
    causal = lax.broadcasted_iota(jnp.int32, (BLOCK, BLOCK), 0) >= lax.broadcasted_iota(
        jnp.int32, (BLOCK, BLOCK), 1
    )
    cum_decay = jnp.einsum("ls,bsgh->blgh", causal.astype(jnp.float32), log_decay, precision=HIGH)
    scaled_x = (conv_xs.reshape(seg_rows, heads_here, HEAD_DIM) * step_size[:, :, None]).reshape(
        blocks, BLOCK, groups_here, group_heads, HEAD_DIM
    )
    b_rows = conv_bs.reshape(blocks, BLOCK, groups_here, STATE)
    c_rows = conv_cs.reshape(blocks, BLOCK, groups_here, STATE)
    block_total = cum_decay[:, BLOCK - 1]
    tail_weight = jnp.exp(block_total[:, None] - cum_decay)
    block_states = jnp.einsum(
        "blgn,blgh,blghp->bghpn", b_rows, tail_weight, scaled_x, precision=HIGH
    )
    block_decay = jnp.exp(block_total)
    total_decay = jnp.exp(jnp.sum(block_total, axis=0))
    start_state = jnp.zeros(block_states.shape[1:], jnp.float32)
    entering, final_state = run_blocks(block_states, block_decay, start_state)
    incoming = carry_in(total_decay, final_state)

    def per_block(run_state, inputs):
        cum_here, b_here, c_here, x_here, fresh_state, factor = inputs
        output = inner_part(cum_here[None], b_here[None], c_here[None], x_here[None], causal)[0]
        output = output + carried_part(c_here[None], run_state[None], cum_here[None])[0]
        return (run_state * factor[:, :, None, None] + fresh_state, output)

    unused, heads_out = lax.scan(
        per_block, incoming, (cum_decay, b_rows, c_rows, scaled_x, block_states, block_decay)
    )
    gated_out = heads_out.reshape(seg_rows, width_x) * jax.nn.silu(gate_rows.astype(jnp.float32))
    grouped = gated_out.reshape(seg_rows, groups_here, width_x // groups_here)
    mixed_rows = ((grouped * inverse_rms(grouped)).reshape(seg_rows, width_x) * gain_here).astype(
        jnp.bfloat16
    )
    partial_sum = jnp.dot(
        mixed_rows,
        lax.all_gather(w_out, "sp", axis=1, tiled=True),
        preferred_element_type=jnp.float32,
    )
    return lax.psum_scatter(partial_sum.astype(jnp.bfloat16), "tp", scatter_dimension=0, tiled=True)


MESH = pl.DeviceIdType.MESH
BF16 = jnp.bfloat16
F32 = jnp.float32
HALO = 16


def mixer_kernel(
    n_sp,
    n_tp,
    tok_ref,
    in_gain_ref,
    w_x_ref,
    w_z_ref,
    w_b_ref,
    w_c_ref,
    w_dt_ref,
    conv_x_ref,
    conv_b_ref,
    conv_c_ref,
    bias_ref,
    a_log_ref,
    gain_ref,
    w_o_ref,
    out_ref,
    nall,
    gath,
    gath_o,
    proj,
    scaled,
    bc_rows,
    log_step,
    cum_seg,
    heads_cum,
    entering,
    state,
    y_buf,
    mixed,
    kept,
    part,
    pair_in,
    slot_f,
    slot_a,
    slot_v,
    tok_send,
    tok_recv,
    halo_send,
    halo_recv,
    z_send,
    x_send,
    w_recv,
    own_sem,
    st_send,
    st_recv,
    cross_send,
    cross_recv,
    rs_send,
    rs_recv,
):
    sp = lax.axis_index("sp")
    tp = lax.axis_index("tp")
    share = tok_ref.shape[0]
    seg_rows = share * n_tp
    blocks = seg_rows // BLOCK
    width = w_x_ref.shape[1]
    half = width // 2
    heads_here = width // HEAD_DIM
    groups_here = half // STATE
    group_heads = heads_here // groups_here
    group_width = width // groups_here
    depth = w_x_ref.shape[0]
    n_z = n_sp // 2
    column = lax.rem(sp, 2)
    plane = sp // 2
    beside = sp + 1 - 2 * column
    own_refs = (w_x_ref, w_b_ref, w_c_ref, w_z_ref, w_o_ref)
    X, B, C, Z, O = range(5)
    X_FIRST = (C,)

    def remote(src, dst, send, recv, where):
        return pltpu.make_async_remote_copy(
            src_ref=src, dst_ref=dst, send_sem=send, recv_sem=recv, device_id=where,
            device_id_type=MESH,
        )

    def place(chunk, source):
        if chunk == O:
            cols = w_o_ref.shape[1]
            return gath_o.at[:, pl.ds(pl.multiple_of(source * cols, cols), cols)]
        rows = pl.ds(pl.multiple_of(source * depth, depth), depth)
        if chunk == X:
            return gath.at[0, rows, :]
        if chunk == Z:
            return gath.at[2, rows, :]
        return gath.at[1, rows, pl.ds(half * (chunk == C), half)]

    upper = plane * 2 // n_z
    mirrored = plane + upper * (n_z - 1 - 2 * plane)

    def plane_at(turn):
        if turn == 0:
            return plane
        near = turn - 1 + (turn + n_z - 1 - mirrored) // n_z
        return near + upper * (n_z - 1 - 2 * near)

    def x_copy(chunk, turn):
        source = 2 * plane_at(turn) + column
        src = own_refs[chunk] if turn == 0 else place(chunk, source)
        return remote(
            src, place(chunk, source), x_send.at[chunk, turn], w_recv.at[chunk, source],
            (beside, tp),
        )

    def z_copy(chunk, other, turn, down):
        side = 1 - column if other else column
        source = 2 * plane_at(turn) + side
        src = own_refs[chunk] if turn == 0 and not other else place(chunk, source)
        target = sp - 2 if down else sp + 2
        return remote(
            src, place(chunk, source), z_send.at[chunk, other, turn, down],
            w_recv.at[chunk, source], (target, tp),
        )

    def arrival(chunk, source):
        return remote(
            own_refs[chunk], place(chunk, source), x_send.at[chunk, 0], w_recv.at[chunk, source],
            (beside, tp),
        )

    def own_copy(chunk):
        return pltpu.make_async_copy(own_refs[chunk], place(chunk, sp), own_sem.at[chunk])

    def along_z(chunk, other, turn, act):
        if turn == 0:
            goes_up = plane < n_z - 1
            goes_down = plane > 0
        else:
            origin = plane_at(turn)
            goes_up = jnp.logical_and(origin < plane, plane < n_z - 1)
            goes_down = jnp.logical_and(origin > plane, plane > 0)

        @pl.when(goes_up)
        def _():
            act(z_copy(chunk, other, turn, 0))

        @pl.when(goes_down)
        def _():
            act(z_copy(chunk, other, turn, 1))

    def start(copy):
        copy.start()

    def launch(chunk):
        x_copy(chunk, 0).start()
        along_z(chunk, 0, 0, start)
        own_copy(chunk).start()

    def pass_on(chunk, turn):
        if chunk in X_FIRST:
            for other in range(2):
                if turn > 0 or other == 1:
                    side = 1 - column if other else column
                    arrival(chunk, 2 * plane_at(turn) + side).wait_recv()
                    along_z(chunk, other, turn, start)
        elif turn > 0:
            arrival(chunk, 2 * plane_at(turn) + column).wait_recv()
            along_z(chunk, 0, turn, start)
            x_copy(chunk, turn).start()

    def forward(chunk):
        for turn in range(n_z):
            pass_on(chunk, turn)

    def finish_plane(chunk, turn):
        if turn == 0:
            own_copy(chunk).wait()
        if chunk not in X_FIRST:
            arrival(chunk, 2 * plane_at(turn) + 1 - column).wait_recv()

    def finish(chunk):
        for turn in range(n_z):
            finish_plane(chunk, turn)

    def drain(chunk):
        for turn in range(n_z):
            if chunk not in X_FIRST or turn == 0:
                x_copy(chunk, turn).wait_send()
            for other in range(1 + (chunk in X_FIRST)):
                along_z(chunk, other, turn, lambda copy: copy.wait_send())

    def token_rows(index):
        return nall.at[pl.ds(pl.multiple_of(HALO + index * share, 16), share), :]

    def token_copy(step):
        return remote(
            token_rows(tp), token_rows(tp), tok_send.at[step - 1], tok_recv.at[tp],
            (sp, lax.rem(tp + step, n_tp)),
        )

    def halo_copy(target):
        return remote(
            nall.at[pl.ds(seg_rows, HALO), :], nall.at[pl.ds(0, HALO), :], halo_send.at[target],
            halo_recv.at[0], (lax.rem(sp + 1, n_sp), target),
        )

    launch(X)
    values = tok_ref[...].astype(F32)
    token_rows(tp)[...] = (values * inverse_rms(values) * in_gain_ref[...]).astype(BF16)

    lanes = log_step.shape[1]
    head_of = lax.broadcasted_iota(jnp.int32, (w_dt_ref.shape[1], lanes), 0)
    lane = lax.broadcasted_iota(jnp.int32, (w_dt_ref.shape[1], lanes), 1)
    pick = jnp.logical_and(head_of == lane + tp * heads_here, lane < heads_here).astype(F32)
    dt_weight = jnp.dot(
        w_dt_ref[...], pick.astype(BF16), preferred_element_type=F32
    ).astype(BF16)
    bias = jnp.dot(bias_ref[...], pick, precision=HIGH, preferred_element_type=F32)
    rate = jnp.dot(jnp.exp(a_log_ref[...]), pick, precision=HIGH, preferred_element_type=F32)
    cols_x = pl.ds(pl.multiple_of(tp * width, width), width)
    cols_b = pl.ds(pl.multiple_of(tp * half, half), half)
    taps_x = conv_x_ref[:, cols_x]
    taps_bc = jnp.concatenate([conv_b_ref[:, cols_b], conv_c_ref[:, cols_b]], axis=1)
    gain = gain_ref[:, cols_x]

    @pl.when(tp == n_tp - 1)
    def _():
        for target in range(n_tp):
            halo_copy(target).start()

    for step in range(1, n_tp):
        token_copy(step).start()
    launch(B)
    launch(C)
    launch(Z)
    forward(X)
    for step in range(1, n_tp):
        source = lax.rem(tp + n_tp - step, n_tp)
        remote(
            token_rows(source), token_rows(source), tok_send.at[0], tok_recv.at[source],
            (sp, source),
        ).wait_recv()
    halo_copy(0).wait_recv()

    @pl.when(tp == n_tp - 1)
    def _():
        for target in range(n_tp):
            halo_copy(target).wait_send()

    for step in range(1, n_tp):
        token_copy(step).wait_send()

    @pl.when(sp == 0)
    def _():
        nall[pl.ds(0, HALO), :] = jnp.zeros((HALO, nall.shape[1]), BF16)

    raw = jnp.dot(nall[pl.ds(HALO, seg_rows), :], dt_weight, preferred_element_type=F32)
    raw = raw + bias
    log_step[...] = jnp.maximum(raw, 0.0) + jnp.log1p(jnp.exp(-jnp.abs(raw)))
    spread = (
        lax.broadcasted_iota(jnp.int32, (lanes, width), 0)
        == lax.broadcasted_iota(jnp.int32, (lanes, width), 1) // HEAD_DIM
    ).astype(F32)
    causal = lax.broadcasted_iota(jnp.int32, (BLOCK, BLOCK), 0) >= lax.broadcasted_iota(
        jnp.int32, (BLOCK, BLOCK), 1
    )

    def project(weights, cols):
        proj[:, cols] = (
            jnp.dot(nall[...], weights, preferred_element_type=F32).astype(BF16).astype(F32)
        )

    def conv(block, taps, cols):
        summed = jnp.zeros((BLOCK, taps.shape[1]), F32)
        first = block * BLOCK + HALO - (CONV - 1)
        for offset in range(CONV):
            summed = summed + taps[offset : offset + 1, :] * proj[
                first + offset : first + offset + BLOCK, cols
            ]
        return summed / (1.0 + jnp.exp(-summed))

    forward(B)
    finish(X)
    project(gath[0], slice(0, width))
    for block in range(blocks):
        rows = pl.ds(block * BLOCK, BLOCK)
        step_here = jnp.dot(log_step[rows, :], spread, precision=HIGH, preferred_element_type=F32)
        scaled[rows, :] = conv(block, taps_x, slice(0, width)) * step_here

    def group_rows(cols):
        project(gath[1, :, cols], cols)
        for block in range(blocks):
            rows = pl.ds(block * BLOCK, BLOCK)
            bc_rows[rows, cols] = conv(block, taps_bc[:, cols], cols).astype(BF16)

    pass_on(C, 0)
    finish(B)
    group_rows(slice(0, half))

    def rows_of(block):
        return pl.ds(pl.multiple_of(block * BLOCK, BLOCK), BLOCK)

    state[...] = jnp.zeros_like(state)
    tri = causal.astype(F32)

    def states_of(block, total):
        rows = rows_of(block)
        log_rate = -log_step[rows, :] * rate
        cum = jnp.dot(tri, log_rate, precision=HIGH, preferred_element_type=F32)
        heads_cum[rows, :] = cum
        wide = jnp.dot(cum, spread, precision=HIGH, preferred_element_type=F32)
        cum_seg[rows, :] = wide
        last = wide[BLOCK - 1 : BLOCK, :]
        weighted = (scaled[rows, :] * jnp.exp(last - wide)).astype(BF16)
        old = state[...]
        entering[block] = old.astype(BF16)
        decay = jnp.exp(last)
        for group in range(groups_here):
            cols = slice(group * group_width, (group + 1) * group_width)
            b_here = bc_rows[rows, group * STATE : (group + 1) * STATE]
            fresh = lax.dot_general(
                b_here, weighted[:, cols], (((0,), (0,)), ((), ())), preferred_element_type=F32
            )
            state[:, cols] = old[:, cols] * decay[:, cols] + fresh
        return total + cum[BLOCK - 1 : BLOCK, :]

    total = lax.fori_loop(0, blocks, states_of, jnp.zeros((1, lanes), F32))
    slot_f[plane] = state[...].astype(BF16)
    slot_a[sp] = jnp.broadcast_to(jnp.exp(total), slot_a.shape[1:])

    def state_copy(source_plane, target_plane):
        return remote(
            slot_f.at[source_plane], slot_f.at[source_plane], st_send.at[0, target_plane],
            st_recv.at[0, source_plane], (2 * target_plane + column, tp),
        )

    def decay_copy(source, target):
        return remote(
            slot_a.at[source], slot_a.at[source], st_send.at[1, target], st_recv.at[1, source],
            (target, tp),
        )

    def to_later(act):
        for target in range(1, n_sp):
            @pl.when(target > sp)
            def _():
                act(decay_copy(sp, target))

        for target in range(1, n_z):
            @pl.when(target > plane)
            def _():
                act(state_copy(plane, target))

    to_later(start)
    launch(O)
    for turn in range(1, n_z):
        pass_on(C, turn)
    finish(C)
    group_rows(slice(half, width))

    def outputs_of(block, carry):
        rows = rows_of(block)
        cum = heads_cum[rows, :]
        cum_t = cum.T
        wide = jnp.exp(cum_seg[rows, :])
        x_here = scaled[rows, :].astype(BF16)
        before = entering[block]
        for group in range(groups_here):
            cols = slice(group * group_width, (group + 1) * group_width)
            b_here = bc_rows[rows, group * STATE : (group + 1) * STATE]
            c_here = bc_rows[rows, half + group * STATE : half + (group + 1) * STATE]
            scores = lax.dot_general(
                c_here, b_here, (((1,), (1,)), ((), ())), preferred_element_type=F32
            )
            parts = []
            for index in range(group * group_heads, (group + 1) * group_heads):
                gap = cum[:, index : index + 1] - cum_t[index : index + 1, :]
                within = jnp.where(causal, jnp.exp(jnp.where(causal, gap, 0.0)), 0.0)
                parts.append(
                    jnp.dot(
                        (scores * within).astype(BF16),
                        x_here[:, index * HEAD_DIM : (index + 1) * HEAD_DIM],
                        preferred_element_type=F32,
                    )
                )
            inner = jnp.concatenate(parts, axis=1)
            carried = jnp.dot(c_here, before[:, cols], preferred_element_type=F32)
            y_buf[rows, cols] = inner + carried * wide[:, cols]
        return carry

    lax.fori_loop(0, blocks, outputs_of, 0)
    forward(Z)

    def decay_of(index):
        return jnp.dot(slot_a[index], spread, precision=HIGH, preferred_element_type=F32)[0:1]

    for source in range(n_sp - 1):
        @pl.when(source < sp)
        def _():
            decay_copy(source, sp).wait_recv()

    state[...] = jnp.zeros_like(state)
    for below in range(n_z - 1):
        @pl.when(below < plane)
        def _():
            state_copy(below, plane).wait_recv()
            after = decay_of(2 * below + 1)
            lead = decay_of(2 * below) * after
            fresh = slot_f[below].astype(F32)

            @pl.when(column == 0)
            def _():
                state[...] = state[...] * lead + fresh * after

            @pl.when(column == 1)
            def _():
                state[...] = state[...] * lead + fresh

    @pl.when(column == 0)
    def _():
        slot_v[0] = (state[...] * decay_of(sp) + slot_f[plane].astype(F32)).astype(BF16)

    @pl.when(column == 1)
    def _():
        slot_v[0] = state[...].astype(BF16)

    cross = remote(slot_v.at[0], slot_v.at[1], cross_send.at[0], cross_recv.at[0], (beside, tp))
    cross.start()
    finish(Z)
    project(gath[2], slice(0, width))
    pass_on(O, 1)
    cross.wait_recv()

    @pl.when(column == 0)
    def _():
        state[...] = state[...] + slot_v[1].astype(F32)

    @pl.when(column == 1)
    def _():
        state[...] = state[...] * decay_of(sp - 1) + slot_v[1].astype(F32)

    def gate_of(block, before):
        rows = rows_of(block)
        wide = cum_seg[rows, :]
        decay = jnp.exp(before + wide)
        gate = proj[pl.ds(pl.multiple_of(block * BLOCK + HALO, 16), BLOCK), :]
        silu = gate / (1.0 + jnp.exp(-gate))
        for group in range(groups_here):
            cols = slice(group * group_width, (group + 1) * group_width)
            c_here = bc_rows[rows, half + group * STATE : half + (group + 1) * STATE]
            carried = jnp.dot(c_here, state[:, cols].astype(BF16), preferred_element_type=F32)
            gated = (y_buf[rows, cols] + carried * decay[:, cols]) * silu[:, cols]
            mixed[rows, cols] = (gated * inverse_rms(gated) * gain[:, cols]).astype(BF16)
        return before + wide[BLOCK - 1 : BLOCK, :]

    lax.fori_loop(0, blocks, gate_of, jnp.zeros((1, width), F32))

    partner = tp + 1 - 2 * lax.rem(tp, 2)
    across = lax.rem(tp + 2, n_tp)
    across_partner = lax.rem(partner + 2, n_tp)
    span = 2 * w_o_ref.shape[1]

    def pair_copy(kind, turn, where):
        return remote(
            part.at[kind, turn], pair_in.at[kind, turn], rs_send.at[kind, turn],
            rs_recv.at[kind, turn], (sp, where),
        )

    def columns_at(turn):
        return pl.ds(pl.multiple_of(plane_at(turn) * span, span), span)

    for turn in range(n_z):
        if 0 < turn < n_z - 1:
            pass_on(O, turn + 1)
        finish_plane(O, turn)
        weights = gath_o[:, columns_at(turn)]

        def product(index):
            rows = pl.ds(pl.multiple_of(index * share, 16), share)
            return (
                jnp.dot(mixed[rows, :], weights, preferred_element_type=F32)
                .astype(BF16)
                .astype(F32)
            )

        part[0, turn] = product(across_partner).astype(BF16)
        pair_copy(0, turn, partner).start()
        part[1, turn] = product(partner).astype(BF16)
        pair_copy(1, turn, partner).start()
        mine = product(across)
        kept[turn] = product(tp)
        pair_copy(0, turn, partner).wait_recv()
        part[2, turn] = (mine + pair_in[0, turn].astype(F32)).astype(BF16)
        pair_copy(2, turn, across).start()

    for turn in range(n_z):
        pair_copy(1, turn, partner).wait_recv()
        pair_copy(2, turn, across).wait_recv()
        whole = kept[turn] + pair_in[1, turn].astype(F32) + pair_in[2, turn].astype(F32)
        out_ref[:, columns_at(turn)] = whole.astype(BF16)

    for turn in range(n_z):
        pair_copy(0, turn, partner).wait_send()
        pair_copy(1, turn, partner).wait_send()
        pair_copy(2, turn, across).wait_send()
    for chunk in range(5):
        drain(chunk)
    to_later(lambda copy: copy.wait_send())
    cross.wait_send()


def fused_body(
    tokens, in_gain, w_x, w_z, w_b, w_c, w_dt, conv_x, conv_b, conv_c, dt_bias, a_log, out_gain,
    w_out,
):
    n_sp = lax.axis_size("sp")
    n_tp = lax.axis_size("tp")
    n_z = n_sp // 2
    share, features = tokens.shape
    seg_rows = share * n_tp
    blocks = seg_rows // BLOCK
    width = w_x.shape[1]
    width_b = w_b.shape[1]
    lanes = 128
    span = features // n_z
    args = (
        tokens, in_gain[None], w_x, w_z, w_b, w_c, w_dt, conv_x, conv_b, conv_c, dt_bias[None],
        a_log[None], out_gain[None], w_out,
    )
    dma = pltpu.SemaphoreType.DMA
    vmem = pltpu.VMEM
    return pl.pallas_call(
        lambda *refs: mixer_kernel(n_sp, n_tp, *refs),
        name="mixer",
        out_shape=jax.ShapeDtypeStruct((share, features), BF16),
        in_specs=[pl.BlockSpec(memory_space=vmem)] * len(args),
        out_specs=pl.BlockSpec(memory_space=vmem),
        scratch_shapes=[
            vmem((seg_rows + HALO, features), BF16),
            vmem((3, features, width), BF16),
            vmem((width, features), BF16),
            vmem((seg_rows + HALO, width), F32),
            vmem((seg_rows, width), F32),
            vmem((seg_rows, 2 * width_b), BF16),
            vmem((seg_rows, lanes), F32),
            vmem((seg_rows, width), F32),
            vmem((seg_rows, lanes), F32),
            vmem((blocks, STATE, width), BF16),
            vmem((STATE, width), F32),
            vmem((seg_rows, width), F32),
            vmem((seg_rows, width), BF16),
            vmem((n_z, share, span), F32),
            vmem((3, n_z, share, span), BF16),
            vmem((3, n_z, share, span), BF16),
            vmem((n_z, STATE, width), BF16),
            vmem((n_sp, 8, lanes), F32),
            vmem((2, STATE, width), BF16),
            dma((n_tp - 1,)),
            dma((n_tp,)),
            dma((n_tp,)),
            dma((1,)),
            dma((5, 2, n_z, 2)),
            dma((5, n_z)),
            dma((5, n_sp)),
            dma((5,)),
            dma((2, n_sp)),
            dma((2, n_sp)),
            dma((1,)),
            dma((1,)),
            dma((3, n_z)),
            dma((3, n_z)),
        ],
        compiler_params=pltpu.CompilerParams(
            has_side_effects=True, vmem_limit_bytes=60 * 1024 * 1024
        ),
    )(*args)


def solution(mesh):
    in_specs = (
        P(("sp", "tp"), None),
        P(),
        P("sp", "tp"),
        P("sp", "tp"),
        P("sp", "tp"),
        P("sp", "tp"),
        P(),
        P(),
        P(),
        P(),
        P(),
        P(),
        P(),
        P("tp", "sp"),
    )
    out_specs = P(("sp", "tp"), None)
    fits = mesh.shape["tp"] == 4 and mesh.shape["sp"] in (4, 6, 8)
    plan = fused_body if fits else body
    return jax.shard_map(plan, mesh=mesh, in_specs=in_specs, out_specs=out_specs, check_vma=False)
```

```python
import jax
import jax.numpy as jnp
from jax import lax
from jax.experimental import pallas as pl
from jax.experimental.pallas import tpu as pltpu
from jax.sharding import PartitionSpec as P

HEAD_DIM = 64
STATE = 128
CONV = 4
BLOCK = 128


EPS = 1e-06
HIGH = lax.Precision.HIGHEST


def carried_in(part, axis, combine, identity):
    place = lax.axis_index(axis)
    gathered = jax.tree.map(lambda a: lax.all_gather(a, axis), part)
    state = jax.tree.map(lambda a, e: jnp.zeros_like(a) + jnp.asarray(e, a.dtype), part, identity)

    def one(lap, state):
        return combine(
            state, jax.tree.map(lambda a: lax.dynamic_index_in_dim(a, lap, 0, False), gathered)
        )

    return lax.fori_loop(0, place, one, state)


def from_behind(value, axis, steps):
    count = lax.axis_size(axis)
    first, last = (max(0, -steps), min(count, count - steps))
    return lax.ppermute(value, axis, [(source, source + steps) for source in range(first, last)])


def inverse_rms(values):
    return lax.rsqrt(jnp.mean(values * values, axis=-1, keepdims=True) + EPS)


def causal_conv(prev_rows, new_rows, kernel):
    joined = jnp.concatenate([prev_rows, new_rows], axis=0).astype(jnp.float32)
    row_count = new_rows.shape[0]
    summed = jnp.zeros(new_rows.shape, jnp.float32)
    for offset in range(kernel.shape[0]):
        summed = summed + kernel[offset] * joined[offset : offset + row_count]
    return jax.nn.silu(summed)


def fold_single(gathered):

    def fold_step(total_part, rows_part, first_row):
        return jnp.dot(gathered, rows_part, preferred_element_type=jnp.float32)

    return fold_step


def fold_products(gathered, totals, weight_rows, first_row):
    single = fold_single(gathered)
    return tuple(
        (
            single(total_part, rows_part, first_row)
            for total_part, rows_part in zip(totals, weight_rows)
        )
    )


def inner_part(cum_decay, b_rows, c_rows, scaled_x, causal):
    scores = jnp.einsum("blgn,bsgn->bgls", c_rows, b_rows, precision=HIGH)
    decay_gap = cum_decay[:, :, None] - cum_decay[:, None, :]
    causal_mask = causal[None, :, :, None, None]
    within = jnp.where(causal_mask, jnp.exp(jnp.where(causal_mask, decay_gap, 0.0)), 0.0)
    return jnp.einsum("bgls,blsgh,bsghp->blghp", scores, within, scaled_x, precision=HIGH)


def carried_part(c_rows, states, cum_decay):
    return jnp.einsum("blgn,bghpn,blgh->blghp", c_rows, states, jnp.exp(cum_decay), precision=HIGH)


def run_blocks(block_states, block_decay, start_state):

    def advance(run_state, inputs):
        fresh_state, factor = inputs
        return (run_state * factor[:, :, None, None] + fresh_state, run_state)

    final_state, entering = lax.scan(advance, start_state, (block_states, block_decay))
    return (entering, final_state)


def chain(earlier, later):
    return (earlier[0] * later[0], earlier[1] * later[0][:, :, None, None] + later[1])


def carry_in(total_decay, final_state):
    identity = (jnp.ones_like(total_decay), jnp.zeros_like(final_state))
    before = carried_in((total_decay, final_state), "sp", chain, identity)
    return before[1]


def body(
    tokens,
    in_gain,
    w_x,
    w_z,
    w_b,
    w_c,
    w_dt,
    conv_x,
    conv_b,
    conv_c,
    dt_bias,
    a_log,
    out_gain,
    w_out,
):
    share_index = lax.axis_index("tp")
    width_x = w_x.shape[1]
    width_b = w_b.shape[1]
    heads_here = width_x // HEAD_DIM
    groups_here = width_b // STATE
    group_heads = heads_here // groups_here
    kernel_x = lax.dynamic_slice_in_dim(conv_x, share_index * width_x, width_x, 1)
    kernel_b = lax.dynamic_slice_in_dim(conv_b, share_index * width_b, width_b, 1)
    kernel_c = lax.dynamic_slice_in_dim(conv_c, share_index * width_b, width_b, 1)
    bias_here = lax.dynamic_slice_in_dim(dt_bias, share_index * heads_here, heads_here, 0)
    rate_here = jnp.exp(lax.dynamic_slice_in_dim(a_log, share_index * heads_here, heads_here, 0))
    gain_here = lax.dynamic_slice_in_dim(out_gain, share_index * width_x, width_x, 0)
    dt_weight = lax.dynamic_slice_in_dim(w_dt, share_index * heads_here, heads_here, 1)
    values = tokens.astype(jnp.float32)
    normed = (values * inverse_rms(values) * in_gain).astype(jnp.bfloat16)
    gathered = lax.all_gather(normed, "tp", axis=0, tiled=True)
    seg_rows = gathered.shape[0]
    blocks = seg_rows // BLOCK
    empty_x = jnp.zeros((seg_rows, width_x), jnp.float32)
    empty_b = jnp.zeros((seg_rows, width_b), jnp.float32)
    projected = fold_products(
        gathered,
        (empty_x, empty_x, empty_b, empty_b),
        (
            lax.all_gather(w_x, "sp", axis=0, tiled=True),
            lax.all_gather(w_z, "sp", axis=0, tiled=True),
            lax.all_gather(w_b, "sp", axis=0, tiled=True),
            lax.all_gather(w_c, "sp", axis=0, tiled=True),
        ),
        jnp.int32(0),
    )
    proj_x, gate_rows, proj_b, proj_c = [
        summed_part.astype(jnp.bfloat16) for summed_part in projected
    ]
    dt_raw = jnp.dot(gathered, dt_weight, preferred_element_type=jnp.float32)
    conv_keep = CONV - 1
    tail_start = seg_rows - conv_keep
    prev_x, prev_b, prev_c = from_behind(
        (proj_x[tail_start:], proj_b[tail_start:], proj_c[tail_start:]), "sp", 1
    )
    conv_xs = causal_conv(prev_x, proj_x, kernel_x)
    conv_bs = causal_conv(prev_b, proj_b, kernel_b)
    conv_cs = causal_conv(prev_c, proj_c, kernel_c)
    step_size = jax.nn.softplus(dt_raw + bias_here)
    log_decay = (-step_size * rate_here).reshape(blocks, BLOCK, groups_here, group_heads)
    causal = lax.broadcasted_iota(jnp.int32, (BLOCK, BLOCK), 0) >= lax.broadcasted_iota(
        jnp.int32, (BLOCK, BLOCK), 1
    )
    cum_decay = jnp.einsum("ls,bsgh->blgh", causal.astype(jnp.float32), log_decay, precision=HIGH)
    scaled_x = (conv_xs.reshape(seg_rows, heads_here, HEAD_DIM) * step_size[:, :, None]).reshape(
        blocks, BLOCK, groups_here, group_heads, HEAD_DIM
    )
    b_rows = conv_bs.reshape(blocks, BLOCK, groups_here, STATE)
    c_rows = conv_cs.reshape(blocks, BLOCK, groups_here, STATE)
    block_total = cum_decay[:, BLOCK - 1]
    tail_weight = jnp.exp(block_total[:, None] - cum_decay)
    block_states = jnp.einsum(
        "blgn,blgh,blghp->bghpn", b_rows, tail_weight, scaled_x, precision=HIGH
    )
    block_decay = jnp.exp(block_total)
    total_decay = jnp.exp(jnp.sum(block_total, axis=0))
    start_state = jnp.zeros(block_states.shape[1:], jnp.float32)
    entering, final_state = run_blocks(block_states, block_decay, start_state)
    incoming = carry_in(total_decay, final_state)

    def per_block(run_state, inputs):
        cum_here, b_here, c_here, x_here, fresh_state, factor = inputs
        output = inner_part(cum_here[None], b_here[None], c_here[None], x_here[None], causal)[0]
        output = output + carried_part(c_here[None], run_state[None], cum_here[None])[0]
        return (run_state * factor[:, :, None, None] + fresh_state, output)

    unused, heads_out = lax.scan(
        per_block, incoming, (cum_decay, b_rows, c_rows, scaled_x, block_states, block_decay)
    )
    gated_out = heads_out.reshape(seg_rows, width_x) * jax.nn.silu(gate_rows.astype(jnp.float32))
    grouped = gated_out.reshape(seg_rows, groups_here, width_x // groups_here)
    mixed_rows = ((grouped * inverse_rms(grouped)).reshape(seg_rows, width_x) * gain_here).astype(
        jnp.bfloat16
    )
    partial_sum = jnp.dot(
        mixed_rows,
        lax.all_gather(w_out, "sp", axis=1, tiled=True),
        preferred_element_type=jnp.float32,
    )
    return lax.psum_scatter(partial_sum.astype(jnp.bfloat16), "tp", scatter_dimension=0, tiled=True)


MESH = pl.DeviceIdType.MESH
BF16 = jnp.bfloat16
F32 = jnp.float32
HALO = 16


def mixer_kernel(
    n_sp,
    n_tp,
    tok_ref,
    in_gain_ref,
    w_x_ref,
    w_z_ref,
    w_b_ref,
    w_c_ref,
    w_dt_ref,
    conv_x_ref,
    conv_b_ref,
    conv_c_ref,
    bias_ref,
    a_log_ref,
    gain_ref,
    w_o_ref,
    out_ref,
    nall,
    gath,
    gath_o,
    proj,
    scaled,
    bc_rows,
    log_step,
    cum_seg,
    heads_cum,
    entering,
    state,
    y_buf,
    mixed,
    kept,
    part,
    pair_in,
    slot_f,
    slot_a,
    slot_v,
    tok_send,
    tok_recv,
    halo_send,
    halo_recv,
    z_send,
    x_send,
    w_recv,
    own_sem,
    st_send,
    st_recv,
    cross_send,
    cross_recv,
    rs_send,
    rs_recv,
):
    sp = lax.axis_index("sp")
    tp = lax.axis_index("tp")
    share = tok_ref.shape[0]
    seg_rows = share * n_tp
    blocks = seg_rows // BLOCK
    width = w_x_ref.shape[1]
    half = width // 2
    heads_here = width // HEAD_DIM
    groups_here = half // STATE
    group_heads = heads_here // groups_here
    group_width = width // groups_here
    depth = w_x_ref.shape[0]
    n_z = n_sp // 2
    column = lax.rem(sp, 2)
    plane = sp // 2
    beside = sp + 1 - 2 * column
    own_refs = (w_x_ref, w_b_ref, w_c_ref, w_z_ref, w_o_ref)
    X, B, C, Z, O = range(5)
    X_FIRST = (C,)

    def remote(src, dst, send, recv, where):
        return pltpu.make_async_remote_copy(
            src_ref=src, dst_ref=dst, send_sem=send, recv_sem=recv, device_id=where,
            device_id_type=MESH,
        )

    def place(chunk, source):
        if chunk == O:
            cols = w_o_ref.shape[1]
            return gath_o.at[:, pl.ds(pl.multiple_of(source * cols, cols), cols)]
        rows = pl.ds(pl.multiple_of(source * depth, depth), depth)
        if chunk == X:
            return gath.at[0, rows, :]
        if chunk == Z:
            return gath.at[2, rows, :]
        return gath.at[1, rows, pl.ds(half * (chunk == C), half)]

    upper = plane * 2 // n_z
    mirrored = plane + upper * (n_z - 1 - 2 * plane)

    def plane_at(turn):
        if turn == 0:
            return plane
        near = turn - 1 + (turn + n_z - 1 - mirrored) // n_z
        return near + upper * (n_z - 1 - 2 * near)

    def x_copy(chunk, turn):
        source = 2 * plane_at(turn) + column
        src = own_refs[chunk] if turn == 0 else place(chunk, source)
        return remote(
            src, place(chunk, source), x_send.at[chunk, turn], w_recv.at[chunk, source],
            (beside, tp),
        )

    def z_copy(chunk, other, turn):
        source = 2 * plane + (1 - column if other else column)
        src = place(chunk, source) if other else own_refs[chunk]
        return remote(
            src, place(chunk, source), z_send.at[chunk, other, turn], w_recv.at[chunk, source],
            (2 * plane_at(turn) + column, tp),
        )

    def relay(chunk):
        origin = plane_at(n_z - 1)
        source = 2 * origin + column
        return remote(
            place(chunk, source), place(chunk, source), z_send.at[chunk, 0, 0],
            w_recv.at[chunk, source], (2 * (n_z - 1 - origin) + column, tp),
        )

    relayed = n_z == 4
    inside = jnp.logical_and(plane > 0, plane < n_z - 1)

    def arrival(chunk, source):
        return remote(
            own_refs[chunk], place(chunk, source), x_send.at[chunk, 0], w_recv.at[chunk, source],
            (beside, tp),
        )

    def own_copy(chunk):
        return pltpu.make_async_copy(own_refs[chunk], place(chunk, sp), own_sem.at[chunk])

    def start(copy):
        copy.start()

    def wait_send(copy):
        copy.wait_send()

    def along_z(chunk, other, act):
        for turn in range(1, n_z):
            if relayed and turn == n_z - 1 and chunk not in X_FIRST:
                @pl.when(inside)
                def _():
                    act(z_copy(chunk, other, turn))
            else:
                act(z_copy(chunk, other, turn))

    def launch(chunk):
        x_copy(chunk, 0).start()
        along_z(chunk, 0, start)
        own_copy(chunk).start()

    def cross_over(chunk):
        arrival(chunk, beside).wait_recv()
        along_z(chunk, 1, start)

    def pass_on(chunk, turn):
        arrival(chunk, 2 * plane_at(turn) + column).wait_recv()
        if relayed and turn == n_z - 1:
            @pl.when(inside)
            def _():
                relay(chunk).start()
        x_copy(chunk, turn).start()

    def finish_plane(chunk, turn):
        if turn == 0:
            own_copy(chunk).wait()
        if chunk not in X_FIRST:
            arrival(chunk, 2 * plane_at(turn) + 1 - column).wait_recv()
        elif turn > 0:
            for side in range(2):
                arrival(chunk, 2 * plane_at(turn) + side).wait_recv()

    def finish(chunk):
        for turn in range(n_z):
            finish_plane(chunk, turn)

    def drain(chunk):
        along_z(chunk, 0, wait_send)
        x_copy(chunk, 0).wait_send()
        if chunk in X_FIRST:
            along_z(chunk, 1, wait_send)
            return
        for turn in range(1, n_z):
            x_copy(chunk, turn).wait_send()
        if relayed:
            @pl.when(inside)
            def _():
                relay(chunk).wait_send()

    def token_rows(index):
        return nall.at[pl.ds(pl.multiple_of(HALO + index * share, 16), share), :]

    def token_copy(step):
        return remote(
            token_rows(tp), token_rows(tp), tok_send.at[step - 1], tok_recv.at[tp],
            (sp, lax.rem(tp + step, n_tp)),
        )

    def halo_copy(target):
        return remote(
            nall.at[pl.ds(seg_rows, HALO), :], nall.at[pl.ds(0, HALO), :], halo_send.at[target],
            halo_recv.at[0], (lax.rem(sp + 1, n_sp), target),
        )

    launch(X)
    values = tok_ref[...].astype(F32)
    token_rows(tp)[...] = (values * inverse_rms(values) * in_gain_ref[...]).astype(BF16)

    lanes = log_step.shape[1]
    heads_all = w_dt_ref.shape[0]

    def picked(shape, head_axis):
        head = lax.broadcasted_iota(jnp.int32, shape, head_axis)
        lane = lax.broadcasted_iota(jnp.int32, shape, 1 - head_axis)
        return jnp.logical_and(head == lane + tp * heads_here, lane < heads_here).astype(F32)

    pick = picked((heads_all, lanes), 0)
    dt_weight = jnp.dot(
        picked((lanes, heads_all), 1).astype(BF16), w_dt_ref[...], preferred_element_type=F32
    ).astype(BF16)
    bias = jnp.dot(bias_ref[...], pick, precision=HIGH, preferred_element_type=F32)
    rate = jnp.dot(jnp.exp(a_log_ref[...]), pick, precision=HIGH, preferred_element_type=F32)
    cols_x = pl.ds(pl.multiple_of(tp * width, width), width)
    cols_b = pl.ds(pl.multiple_of(tp * half, half), half)
    taps_x = conv_x_ref[:, cols_x]
    taps_bc = jnp.concatenate([conv_b_ref[:, cols_b], conv_c_ref[:, cols_b]], axis=1)
    gain = gain_ref[:, cols_x]

    @pl.when(tp == n_tp - 1)
    def _():
        for target in range(n_tp):
            halo_copy(target).start()

    for step in range(1, n_tp):
        token_copy(step).start()
    launch(B)
    launch(C)

    def forward(chunk):
        for turn in range(1, n_z):
            pass_on(chunk, turn)

    forward(X)
    cross_over(C)
    launch(Z)
    for step in range(1, n_tp):
        source = lax.rem(tp + n_tp - step, n_tp)
        remote(
            token_rows(source), token_rows(source), tok_send.at[0], tok_recv.at[source],
            (sp, source),
        ).wait_recv()
    halo_copy(0).wait_recv()

    @pl.when(tp == n_tp - 1)
    def _():
        for target in range(n_tp):
            halo_copy(target).wait_send()

    for step in range(1, n_tp):
        token_copy(step).wait_send()

    @pl.when(sp == 0)
    def _():
        nall[pl.ds(0, HALO), :] = jnp.zeros((HALO, nall.shape[1]), BF16)

    raw = lax.dot_general(
        nall[pl.ds(HALO, seg_rows), :], dt_weight, (((1,), (1,)), ((), ())),
        preferred_element_type=F32,
    )
    raw = raw + bias
    log_step[...] = jnp.maximum(raw, 0.0) + jnp.log1p(jnp.exp(-jnp.abs(raw)))
    spread = (
        lax.broadcasted_iota(jnp.int32, (lanes, width), 0)
        == lax.broadcasted_iota(jnp.int32, (lanes, width), 1) // HEAD_DIM
    ).astype(F32)
    causal = lax.broadcasted_iota(jnp.int32, (BLOCK, BLOCK), 0) >= lax.broadcasted_iota(
        jnp.int32, (BLOCK, BLOCK), 1
    )

    def project(weights, cols):
        proj[:, cols] = (
            jnp.dot(nall[...], weights, preferred_element_type=F32).astype(BF16).astype(F32)
        )

    def conv(block, taps, cols):
        summed = jnp.zeros((BLOCK, taps.shape[1]), F32)
        first = block * BLOCK + HALO - (CONV - 1)
        for offset in range(CONV):
            summed = summed + taps[offset : offset + 1, :] * proj[
                first + offset : first + offset + BLOCK, cols
            ]
        return summed / (1.0 + jnp.exp(-summed))

    forward(B)
    finish(X)
    project(gath[0], slice(0, width))
    for block in range(blocks):
        rows = pl.ds(block * BLOCK, BLOCK)
        step_here = jnp.dot(log_step[rows, :], spread, precision=HIGH, preferred_element_type=F32)
        scaled[rows, :] = conv(block, taps_x, slice(0, width)) * step_here

    def group_rows(cols):
        project(gath[1, :, cols], cols)
        for block in range(blocks):
            rows = pl.ds(block * BLOCK, BLOCK)
            bc_rows[rows, cols] = conv(block, taps_bc[:, cols], cols).astype(BF16)

    for turn in range(1, n_z - 1):
        pass_on(Z, turn)
    finish(B)
    group_rows(slice(0, half))

    def rows_of(block):
        return pl.ds(pl.multiple_of(block * BLOCK, BLOCK), BLOCK)

    state[...] = jnp.zeros_like(state)
    tri = causal.astype(F32)

    def states_of(block, total):
        rows = rows_of(block)
        log_rate = -log_step[rows, :] * rate
        cum = jnp.dot(tri, log_rate, precision=HIGH, preferred_element_type=F32)
        heads_cum[rows, :] = cum
        wide = jnp.dot(cum, spread, precision=HIGH, preferred_element_type=F32)
        cum_seg[rows, :] = wide
        last = wide[BLOCK - 1 : BLOCK, :]
        weighted = (scaled[rows, :] * jnp.exp(last - wide)).astype(BF16)
        old = state[...]
        entering[block] = old.astype(BF16)
        decay = jnp.exp(last)
        for group in range(groups_here):
            cols = slice(group * group_width, (group + 1) * group_width)
            b_here = bc_rows[rows, group * STATE : (group + 1) * STATE]
            fresh = lax.dot_general(
                b_here, weighted[:, cols], (((0,), (0,)), ((), ())), preferred_element_type=F32
            )
            state[:, cols] = old[:, cols] * decay[:, cols] + fresh
        return total + cum[BLOCK - 1 : BLOCK, :]

    total = lax.fori_loop(0, blocks, states_of, jnp.zeros((1, lanes), F32))
    slot_f[plane] = state[...].astype(BF16)
    slot_a[sp] = jnp.broadcast_to(jnp.exp(total), slot_a.shape[1:])

    def state_copy(source_plane, target_plane):
        return remote(
            slot_f.at[source_plane], slot_f.at[source_plane], st_send.at[0, target_plane],
            st_recv.at[0, source_plane], (2 * target_plane + column, tp),
        )

    def decay_copy(source, target):
        return remote(
            slot_a.at[source], slot_a.at[source], st_send.at[1, target], st_recv.at[1, source],
            (target, tp),
        )

    def to_later(act):
        for target in range(1, n_sp):
            @pl.when(target > sp)
            def _():
                act(decay_copy(sp, target))

        for target in range(1, n_z):
            @pl.when(target > plane)
            def _():
                act(state_copy(plane, target))

    to_later(start)
    launch(O)
    pass_on(Z, n_z - 1)
    finish(C)
    group_rows(slice(half, width))

    def outputs_of(block, carry):
        rows = rows_of(block)
        cum = heads_cum[rows, :]
        cum_t = cum.T
        wide = jnp.exp(cum_seg[rows, :])
        x_here = scaled[rows, :].astype(BF16)
        before = entering[block]
        for group in range(groups_here):
            cols = slice(group * group_width, (group + 1) * group_width)
            b_here = bc_rows[rows, group * STATE : (group + 1) * STATE]
            c_here = bc_rows[rows, half + group * STATE : half + (group + 1) * STATE]
            scores = lax.dot_general(
                c_here, b_here, (((1,), (1,)), ((), ())), preferred_element_type=F32
            )
            parts = []
            for index in range(group * group_heads, (group + 1) * group_heads):
                gap = cum[:, index : index + 1] - cum_t[index : index + 1, :]
                within = jnp.where(causal, jnp.exp(jnp.where(causal, gap, 0.0)), 0.0)
                parts.append(
                    jnp.dot(
                        (scores * within).astype(BF16),
                        x_here[:, index * HEAD_DIM : (index + 1) * HEAD_DIM],
                        preferred_element_type=F32,
                    )
                )
            inner = jnp.concatenate(parts, axis=1)
            carried = jnp.dot(c_here, before[:, cols], preferred_element_type=F32)
            y_buf[rows, cols] = inner + carried * wide[:, cols]
        return carry

    lax.fori_loop(0, blocks, outputs_of, 0)
    pass_on(O, 1)

    def decay_of(index):
        return jnp.dot(slot_a[index], spread, precision=HIGH, preferred_element_type=F32)[0:1]

    for source in range(n_sp - 1):
        @pl.when(source < sp)
        def _():
            decay_copy(source, sp).wait_recv()

    state[...] = jnp.zeros_like(state)
    for below in range(n_z - 1):
        @pl.when(below < plane)
        def _():
            state_copy(below, plane).wait_recv()
            after = decay_of(2 * below + 1)
            lead = decay_of(2 * below) * after
            fresh = slot_f[below].astype(F32)

            @pl.when(column == 0)
            def _():
                state[...] = state[...] * lead + fresh * after

            @pl.when(column == 1)
            def _():
                state[...] = state[...] * lead + fresh

    @pl.when(column == 0)
    def _():
        slot_v[0] = (state[...] * decay_of(sp) + slot_f[plane].astype(F32)).astype(BF16)

    @pl.when(column == 1)
    def _():
        slot_v[0] = state[...].astype(BF16)

    cross = remote(slot_v.at[0], slot_v.at[1], cross_send.at[0], cross_recv.at[0], (beside, tp))
    cross.start()
    finish(Z)
    project(gath[2], slice(0, width))
    cross.wait_recv()

    @pl.when(column == 0)
    def _():
        state[...] = state[...] + slot_v[1].astype(F32)

    @pl.when(column == 1)
    def _():
        state[...] = state[...] * decay_of(sp - 1) + slot_v[1].astype(F32)

    def gate_of(block, before):
        rows = rows_of(block)
        wide = cum_seg[rows, :]
        decay = jnp.exp(before + wide)
        gate = proj[pl.ds(pl.multiple_of(block * BLOCK + HALO, 16), BLOCK), :]
        silu = gate / (1.0 + jnp.exp(-gate))
        for group in range(groups_here):
            cols = slice(group * group_width, (group + 1) * group_width)
            c_here = bc_rows[rows, half + group * STATE : half + (group + 1) * STATE]
            carried = jnp.dot(c_here, state[:, cols].astype(BF16), preferred_element_type=F32)
            gated = (y_buf[rows, cols] + carried * decay[:, cols]) * silu[:, cols]
            mixed[rows, cols] = (gated * inverse_rms(gated) * gain[:, cols]).astype(BF16)
        return before + wide[BLOCK - 1 : BLOCK, :]

    lax.fori_loop(0, blocks, gate_of, jnp.zeros((1, width), F32))

    partner = tp + 1 - 2 * lax.rem(tp, 2)
    across = lax.rem(tp + 2, n_tp)
    across_partner = lax.rem(partner + 2, n_tp)
    span = 2 * w_o_ref.shape[1]

    def pair_copy(kind, turn, where):
        return remote(
            part.at[kind, turn], pair_in.at[kind, turn], rs_send.at[kind, turn],
            rs_recv.at[kind, turn], (sp, where),
        )

    def columns_at(turn):
        return pl.ds(pl.multiple_of(plane_at(turn) * span, span), span)

    for turn in range(n_z):
        if 0 < turn < n_z - 1:
            pass_on(O, turn + 1)
        finish_plane(O, turn)
        weights = gath_o[:, columns_at(turn)]

        def product(index):
            rows = pl.ds(pl.multiple_of(index * share, 16), share)
            return (
                jnp.dot(mixed[rows, :], weights, preferred_element_type=F32)
                .astype(BF16)
                .astype(F32)
            )

        part[0, turn] = product(across_partner).astype(BF16)
        pair_copy(0, turn, partner).start()
        part[1, turn] = product(partner).astype(BF16)
        pair_copy(1, turn, partner).start()
        mine = product(across)
        kept[turn] = product(tp)
        pair_copy(0, turn, partner).wait_recv()
        part[2, turn] = (mine + pair_in[0, turn].astype(F32)).astype(BF16)
        pair_copy(2, turn, across).start()

    for turn in range(n_z):
        pair_copy(1, turn, partner).wait_recv()
        pair_copy(2, turn, across).wait_recv()
        whole = kept[turn] + pair_in[1, turn].astype(F32) + pair_in[2, turn].astype(F32)
        out_ref[:, columns_at(turn)] = whole.astype(BF16)

    for turn in range(n_z):
        pair_copy(0, turn, partner).wait_send()
        pair_copy(1, turn, partner).wait_send()
        pair_copy(2, turn, across).wait_send()
    for chunk in range(5):
        drain(chunk)
    to_later(lambda copy: copy.wait_send())
    cross.wait_send()


def fused_body(
    tokens, in_gain, w_x, w_z, w_b, w_c, w_dt, conv_x, conv_b, conv_c, dt_bias, a_log, out_gain,
    w_out,
):
    n_sp = lax.axis_size("sp")
    n_tp = lax.axis_size("tp")
    n_z = n_sp // 2
    share, features = tokens.shape
    seg_rows = share * n_tp
    blocks = seg_rows // BLOCK
    width = w_x.shape[1]
    width_b = w_b.shape[1]
    lanes = 128
    span = features // n_z
    args = (
        tokens, in_gain[None], w_x, w_z, w_b, w_c, w_dt.T, conv_x, conv_b, conv_c, dt_bias[None],
        a_log[None], out_gain[None], w_out,
    )
    dma = pltpu.SemaphoreType.DMA
    vmem = pltpu.VMEM
    return pl.pallas_call(
        lambda *refs: mixer_kernel(n_sp, n_tp, *refs),
        name="mixer",
        out_shape=jax.ShapeDtypeStruct((share, features), BF16),
        in_specs=[pl.BlockSpec(memory_space=vmem)] * len(args),
        out_specs=pl.BlockSpec(memory_space=vmem),
        scratch_shapes=[
            vmem((seg_rows + HALO, features), BF16),
            vmem((3, features, width), BF16),
            vmem((width, features), BF16),
            vmem((seg_rows + HALO, width), F32),
            vmem((seg_rows, width), F32),
            vmem((seg_rows, 2 * width_b), BF16),
            vmem((seg_rows, lanes), F32),
            vmem((seg_rows, width), F32),
            vmem((seg_rows, lanes), F32),
            vmem((blocks, STATE, width), BF16),
            vmem((STATE, width), F32),
            vmem((seg_rows, width), F32),
            vmem((seg_rows, width), BF16),
            vmem((n_z, share, span), F32),
            vmem((3, n_z, share, span), BF16),
            vmem((3, n_z, share, span), BF16),
            vmem((n_z, STATE, width), BF16),
            vmem((n_sp, 8, lanes), F32),
            vmem((2, STATE, width), BF16),
            dma((n_tp - 1,)),
            dma((n_tp,)),
            dma((n_tp,)),
            dma((1,)),
            dma((5, 2, n_z)),
            dma((5, n_z)),
            dma((5, n_sp)),
            dma((5,)),
            dma((2, n_sp)),
            dma((2, n_sp)),
            dma((1,)),
            dma((1,)),
            dma((3, n_z)),
            dma((3, n_z)),
        ],
        compiler_params=pltpu.CompilerParams(
            has_side_effects=True, vmem_limit_bytes=60 * 1024 * 1024
        ),
    )(*args)


def solution(mesh):
    in_specs = (
        P(("sp", "tp"), None),
        P(),
        P("sp", "tp"),
        P("sp", "tp"),
        P("sp", "tp"),
        P("sp", "tp"),
        P(),
        P(),
        P(),
        P(),
        P(),
        P(),
        P(),
        P("tp", "sp"),
    )
    out_specs = P(("sp", "tp"), None)
    fits = mesh.shape["tp"] == 4 and mesh.shape["sp"] in (4, 6, 8)
    plan = fused_body if fits else body
    return jax.shard_map(plan, mesh=mesh, in_specs=in_specs, out_specs=out_specs, check_vma=False)
```
